32 devices in a mesh: grp: 2 (over y), ra: 4 (over z), cb: 4 (over x, core).
Axes of the slice: x: 2, y: 2, z: 4, core: 2. Of those that a mesh axis runs over, the one named last changes fastest.
Arguments:
- residual: bfloat16 [512, 4096], P('grp', 'ra'), parts along dimension 0, may hold values from -6 to 6
- gain_first: bfloat16 [4096], P('ra'), may hold values from 0.099609375 to 1.8984375
- gate_first: bfloat16 [4096, 11264], P('ra', 'cb'), may hold values from -0.09375 to 0.09375
- up_first: bfloat16 [4096, 11264], P('ra', 'cb'), may hold values from -0.09375 to 0.09375
- down_first: bfloat16 [11264, 4096], P('cb', 'ra'), may hold values from -0.078125 to 0.078125
- gain_second: bfloat16 [4096], P('ra'), may hold values from 0.099609375 to 1.8984375
- gate_second: bfloat16 [4096, 11264], P('ra', 'cb'), may hold values from -0.09375 to 0.09375
- up_second: bfloat16 [4096, 11264], P('ra', 'cb'), may hold values from -0.09375 to 0.09375
- down_second: bfloat16 [11264, 4096], P('cb', 'ra'), may hold values from -0.078125 to 0.078125
Outputs:
- updated: bfloat16 [512, 4096], P('grp', 'ra'), parts along dimension 0
The draws below stay inside these ranges and needn't reach their ends.
There are 2 independent parts, one for each index of `grp`. The reference program is written for one: setup_inputs(seed, part) draws one part's arguments, and reference() takes and returns one part's arrays. A program takes and returns all parts, laid end to end along the dimension named above; an argument that names none is the same for every part. Nothing has to cross between parts.
All inputs are finite; a program needn't handle non-finite values.
Results may differ from the reference program's by a relative error of at most 0.0071.
Values may be sent and summed in bfloat16 or wider, within the bound.
A program may use at most 128 MiB of HBM per device.

```python
import jax
import jax.numpy as jnp
from jax import lax

D = 4096
FF = 11264
TOK = 256


def draw_residual(key, part):
    first, second, third = jax.random.split(jax.random.fold_in(key, 11), 3)
    rows = jnp.exp(jax.random.uniform(first, (TOK, 1), jnp.float32, jnp.log(0.25), jnp.log(2.5)))
    ramp = jnp.exp(jnp.linspace(jnp.log(0.5), jnp.log(2.0), D)).astype(jnp.float32)
    columns = ramp[None, :] * jnp.exp(jax.random.uniform(third, (1, D), jnp.float32, -0.3, 0.3))
    base = jnp.clip(jax.random.normal(second, (TOK, D), jnp.float32), -4.0, 4.0)
    return jnp.clip(0.4 * rows * columns * base, -6.0, 6.0).astype(jnp.bfloat16)


def spiked(values, stream_key, source, target, blocks, factor):
    def block_of(position):
        return (jnp.arange(values.shape[position]) // (values.shape[position] // blocks)).reshape((-1,) + (1,) * (values.ndim - 1 - position))

    near = jax.random.permutation(stream_key, blocks)[block_of(target)]
    far = (block_of(target) + blocks // 2) % blocks
    return jnp.where((block_of(source) == near) | (block_of(source) == far), factor * values, values)


def level_of(own_key, extent, cuts, smallest, high):
    def one(position, shards_of):
        heights = jax.random.uniform(jax.random.fold_in(jax.random.fold_in(own_key, 6), position), (shards_of,), jnp.float32, smallest / len(cuts), high / len(cuts))
        return jnp.repeat(jnp.exp(heights), extent[position] // shards_of).reshape((-1,) + (1,) * (len(extent) - position - 1))

    level = one(*cuts[0])
    for cut in cuts[1:]:
        level = level * one(*cut)
    return level


def bell_draw(stream_key, extent, width, reach, pieces=(), kind=jnp.bfloat16):
    level = level_of(stream_key, extent, pieces, -0.22, 0.18) if pieces else 1.0
    array = jax.random.normal(stream_key, extent, jnp.float32) * width * level
    return jnp.minimum(jnp.maximum(array, -reach), reach).astype(kind)


def heavy_noise(own_key, extent, width, bound, shards, heavy, held_as=jnp.bfloat16):
    drawn = width * jax.random.normal(own_key, extent, jnp.float32)
    if shards:
        drawn = drawn * level_of(own_key, extent, shards, -0.22, 0.18)
    return jnp.clip(spiked(drawn, jax.random.fold_in(own_key, 3), *heavy), -bound, bound).astype(held_as)


def setup_inputs(seed: int = 0, part: int = 0) -> dict:
    arg_keys = jax.random.split(jax.random.key(seed), 10)
    part_splits = jax.random.split(jax.random.fold_in(arg_keys[9], part), 10)
    residual = draw_residual(jax.random.fold_in(jax.random.fold_in(arg_keys[9], part), 71), part)
    gain_first = jnp.clip(1.0 + 0.18 * jax.random.normal(arg_keys[1], (D,), jnp.float32), 0.099609375, 1.8984375).astype(jnp.bfloat16)
    gate_first = bell_draw(arg_keys[2], (D, FF), D ** -0.5, 0.09375, ((0, 4), (1, 4)))
    up_first = bell_draw(arg_keys[3], (D, FF), D ** -0.5, 0.09375, ((0, 4), (1, 4)))
    down_first = heavy_noise(arg_keys[4], (FF, D), FF ** -0.5, 0.078125, ((0, 4), (1, 4)), (0, 1, 4, 2.0))
    gain_second = jnp.clip(1.0 + 0.18 * jax.random.normal(arg_keys[5], (D,), jnp.float32), 0.099609375, 1.8984375).astype(jnp.bfloat16)
    gate_second = bell_draw(arg_keys[6], (D, FF), D ** -0.5, 0.09375, ((0, 4), (1, 4)))
    up_second = bell_draw(arg_keys[7], (D, FF), D ** -0.5, 0.09375, ((0, 4), (1, 4)))
    down_second = heavy_noise(arg_keys[8], (FF, D), FF ** -0.5, 0.078125, ((0, 4), (1, 4)), (0, 1, 4, 2.0))
    return dict(residual=residual, gain_first=gain_first, gate_first=gate_first, up_first=up_first, down_first=down_first, gain_second=gain_second, gate_second=gate_second, up_second=up_second, down_second=down_second)


epsilon = 1e-06

def half_step(stream, gain, w_gate, w_up, w_down):
    values = stream.astype(jnp.float32)
    scale = lax.rsqrt(lax.optimization_barrier(jnp.mean(values * values, axis=1, keepdims=True)) + epsilon)
    normed = (values * gain.astype(jnp.float32)).astype(jnp.bfloat16)
    gate = scale * jnp.dot(normed, w_gate, preferred_element_type=jnp.float32)
    upward = scale * jnp.dot(normed, w_up, preferred_element_type=jnp.float32)
    hidden = (jax.nn.silu(gate) * upward).astype(jnp.bfloat16)
    branch = jnp.dot(hidden, w_down, preferred_element_type=jnp.float32)
    return (values + 0.5 * branch).astype(jnp.bfloat16)

def reference(residual, gain_first, gate_first, up_first, down_first, gain_second, gate_second, up_second, down_second):
    middle = half_step(residual, gain_first, gate_first, up_first, down_first)
    return half_step(middle, gain_second, gate_second, up_second, down_second)
```

```python
import functools

import jax
import jax.numpy as jnp
from jax import lax
from jax.experimental import pallas as pl
from jax.experimental.pallas import tpu as pltpu
from jax.sharding import PartitionSpec as P

MESH = pl.DeviceIdType.MESH
LANES = 128
epsilon = 1e-06

HOP = 4
REDUCE = 4
SPREAD = 4
TILE = 8
AHEAD = 3
LOADS = 6
BEHIND = 4
WIDE = 2
DEEP = 4


def kernel(
    cfg,
    residual,
    gain_first,
    gain_second,
    gate_first,
    up_first,
    down_first,
    gate_second,
    up_second,
    down_second,
    out,
    w_in,
    w_down,
    stream_in,
    normed_one,
    normed,
    own,
    part_out,
    part_in,
    hidden,
    total,
    rs_own,
    rs_out,
    rs_in,
    merged,
    sq_own,
    sq_out,
    sq_in,
    scale,
    w_sem,
    x_sem,
    out_sem,
    part_send,
    part_recv,
    hid_send,
    hid_recv,
    sq_send,
    sq_recv,
    rs_send,
    rs_recv,
    ag_send,
    ag_recv,
):
    R, C, blocks, pieces, width, rows, gap, model = cfg
    per_phase = blocks * pieces
    count = 2 * per_phase
    r = lax.axis_index("ra")
    c = lax.axis_index("cb")

    gates, ups, downs = (gate_first, gate_second), (up_first, up_second), (down_first, down_second)

    def weight_copy(phase, p, which):
        span = pl.ds(p * width if pieces > 1 else 0, width)
        if which == 2:
            return pltpu.make_async_copy(
                downs[phase].at[span, :], w_down.at[phase, p], w_sem.at[phase, 2, p]
            )
        source = (gates, ups)[which][phase]
        return pltpu.make_async_copy(
            source.at[:, span], w_in.at[phase, p, which], w_sem.at[phase, which, p]
        )

    stream_copy = pltpu.make_async_copy(residual, stream_in, x_sem)
    stream_copy.start()
    for p in range(min(AHEAD, pieces)):
        weight_copy(0, p, 0).start()
        weight_copy(0, p, 1).start()

    def load_rest(s):
        def at(first_step, first_piece, phase, kinds):
            p = s - first_step + first_piece

            @pl.when((p >= first_piece) & (p < pieces))
            def _():
                for which in kinds:
                    weight_copy(phase, p, which).start()

        at(0, AHEAD, 0, (0, 1))
        at(LOADS, 0, 0, (2,))
        at(LOADS + pieces, 0, 1, (0, 1))
        at(LOADS + 2 * pieces, 0, 1, (2,))

    barrier = pltpu.get_barrier_semaphore()

    @pl.when(r > 0)
    def _():
        pl.semaphore_signal(barrier, inc=1, device_id={"ra": r - 1}, device_id_type=MESH)

    @pl.when(r < R - 1)
    def _():
        pl.semaphore_signal(barrier, inc=1, device_id={"ra": r + 1}, device_id_type=MESH)

    for k in range(1, C):
        pl.semaphore_signal(
            barrier, inc=1, device_id={"cb": lax.rem(c + k, C)}, device_id_type=MESH
        )

    def diagonal():
        shape = (rows, rows)
        return lax.broadcasted_iota(jnp.int32, shape, 0) == lax.broadcasted_iota(jnp.int32, shape, 1)

    def scaled(stream, gain_ref):
        values = stream.astype(jnp.float32)
        square = jnp.sum(values * values, axis=1, keepdims=True)
        gain = gain_ref[...].astype(jnp.float32).reshape(1, -1)
        return (values * gain).astype(jnp.bfloat16), square

    def keep_square(phase, block, square):
        line = jnp.sum(jnp.where(diagonal(), square, 0.0), axis=0, keepdims=True)
        sq_own[phase, block] = jnp.broadcast_to(line, (TILE, rows))

    stream_copy.wait()
    for block in range(blocks):
        normed_one[pl.ds(block * rows, rows)], square = scaled(
            stream_in[block].reshape(rows, -1), gain_first
        )
        keep_square(0, block, square)

    near = jnp.where(r > 0, 1, 0) + jnp.where(r < R - 1, 1, 0)
    pl.semaphore_wait(barrier, C - 1 + near)

    place = (r, R - 1 - r)
    onward = (r + 1, r - 1)
    back = (r - 1, r + 1)

    def part_copy(d, i):
        return pltpu.make_async_remote_copy(
            src_ref=part_out.at[i],
            dst_ref=part_in.at[i],
            send_sem=part_send.at[i],
            recv_sem=part_recv.at[i],
            device_id={"ra": onward[d]},
            device_id_type=MESH,
        )

    def square_copy(d, pb):
        return pltpu.make_async_remote_copy(
            src_ref=sq_out.at[pb, d],
            dst_ref=sq_in.at[pb, d],
            send_sem=sq_send.at[d, pb],
            recv_sem=sq_recv.at[d, pb],
            device_id={"ra": onward[d]},
            device_id_type=MESH,
        )

    def hidden_copy(d, i):
        return pltpu.make_async_remote_copy(
            src_ref=hidden.at[i],
            dst_ref=hidden.at[i],
            send_sem=hid_send.at[i],
            recv_sem=hid_recv.at[i],
            device_id={"ra": back[d]},
            device_id_type=MESH,
        )

    def squares_went(d, pb):
        return (pieces > 1) | (lax.rem(pb, 2) == d)

    def reduce_copy(pb, k):
        peer = lax.rem(c + k, C)
        return pltpu.make_async_remote_copy(
            src_ref=rs_out.at[pb, peer],
            dst_ref=rs_in.at[pb, k - 1],
            send_sem=rs_send.at[pb, k - 1],
            recv_sem=rs_recv.at[pb, k - 1],
            device_id={"cb": peer},
            device_id_type=MESH,
        )

    def spread_copy(pb, k):
        return pltpu.make_async_remote_copy(
            src_ref=merged.at[pb, c],
            dst_ref=merged.at[pb, c],
            send_sem=ag_send.at[pb, k - 1],
            recv_sem=ag_recv.at[pb, k - 1],
            device_id={"cb": lax.rem(c + k, C)},
            device_id_type=MESH,
        )

    def out_copy(block):
        return pltpu.make_async_copy(
            merged.at[blocks + block], out.at[block], out_sem.at[block]
        )

    def at_step(slot, body, side=None):
        early = (slot >= 0) & (slot < per_phase)
        late = (slot >= per_phase + gap) & (slot < count + gap)

        @pl.when(early | late)
        def _():
            phase = jnp.where(late, 1, 0)
            i = slot - phase * gap
            local = i - phase * per_phase
            block = lax.div(local, pieces)
            p = lax.rem(local, pieces)
            if side is None:
                body(i, phase, block, p)
            else:

                @pl.when(lax.rem(i, 2) == side)
                def _():
                    body(i, phase, block, p)

    def both_phases(phase, body):
        for static in range(2):

            @pl.when(phase == static)
            def _():
                body(static)

    def project_one(s):
        @pl.when(s < pieces)
        def _():
            for which in range(2):
                weight_copy(0, s, which).wait()
            x = normed_one[...]
            for which in range(2):
                product = jnp.dot(x, w_in[0, s, which], preferred_element_type=jnp.float32)
                for block in range(blocks):
                    own[block * pieces + s, which] = product[block * rows : (block + 1) * rows]

    def project_two(s):
        local = s - per_phase - gap

        @pl.when((local >= 0) & (local < per_phase))
        def _():
            block = lax.div(local, pieces)
            p = lax.rem(local, pieces)

            def some(count_of):
                @pl.when(block == 0)
                def _():
                    for q in range(count_of):
                        weight_copy(1, p + q, 0).wait()
                        weight_copy(1, p + q, 1).wait()

                x = normed[block]
                for q in range(count_of):
                    for which in range(2):
                        own[local + q, which] = jnp.dot(
                            x, w_in[1, p + q, which], preferred_element_type=jnp.float32
                        )

            left = pieces % WIDE

            @pl.when((lax.rem(p, WIDE) == 0) & (p + WIDE <= pieces))
            def _():
                some(WIDE)

            if left:

                @pl.when(p == pieces - left)
                def _():
                    some(left)

    def forward(d):
        def body(i, phase, block, p):
            slot = i - phase * per_phase
            pb = phase * blocks + block
            opening = p < 2
            old = i - 2 * BEHIND

            @pl.when((place[d] < R - 1) & (old >= 0))
            def _():
                part_copy(d, old).wait_send()

            @pl.when(place[d] == 0)
            def _():
                part_out[i] = own[slot].astype(jnp.bfloat16)
                part_copy(d, i).start()

                @pl.when(opening)
                def _():
                    sq_out[pb, d] = sq_own[phase, block]
                    square_copy(d, pb).start()

            @pl.when((place[d] > 0) & (place[d] < R - 1))
            def _():
                part_copy(d, i).wait_recv()
                part_out[i] = (own[slot] + part_in[i].astype(jnp.float32)).astype(jnp.bfloat16)
                part_copy(d, i).start()

                @pl.when(opening)
                def _():
                    square_copy(d, pb).wait_recv()
                    sq_out[pb, d] = sq_own[phase, block] + sq_in[pb, d]
                    square_copy(d, pb).start()

            @pl.when(place[d] == R - 1)
            def _():
                @pl.when(opening)
                def _():
                    square_copy(d, pb).wait_recv()
                    mean = (sq_own[phase, block] + sq_in[pb, d])[:1] / model
                    line = lax.rsqrt(mean + epsilon)
                    column = jnp.sum(jnp.where(diagonal(), line, 0.0), axis=1, keepdims=True)
                    scale[d] = jnp.broadcast_to(column, (rows, LANES))

                part_copy(d, i).wait_recv()
                factor = scale[d][:, :1]
                gate = (own[slot, 0] + part_in[i, 0].astype(jnp.float32)) * factor
                up = (own[slot, 1] + part_in[i, 1].astype(jnp.float32)) * factor
                hidden[i] = (gate / (1.0 + jnp.exp(-gate)) * up).astype(jnp.bfloat16)
                hidden_copy(d, i).start()

                @pl.when(old >= 0)
                def _():
                    hidden_copy(d, old).wait_send()

        return body

    def pass_back(d):
        def body(i, phase, block, p):
            @pl.when(place[d] < R - 1)
            def _():
                hidden_copy(d, i).wait_recv()

                @pl.when(place[d] > 0)
                def _():
                    hidden_copy(d, i).start()

                    @pl.when(i >= 2 * BEHIND)
                    def _():
                        hidden_copy(d, i - 2 * BEHIND).wait_send()

        return body

    def down(i, phase, block, p):
        pb = phase * blocks + block

        def some(count_of):
            start = p - count_of + 1
            slot = i - count_of + 1

            @pl.when(block == 0)
            def _():
                for q in range(count_of):
                    both_phases(phase, lambda static: weight_copy(static, start + q, 2).wait())

            product = jnp.dot(
                jnp.concatenate([hidden[slot + q] for q in range(count_of)], axis=1),
                w_down[phase, pl.ds(start, count_of)].reshape(count_of * width, -1),
                preferred_element_type=jnp.float32,
            ).reshape(total.shape)

            @pl.when(start == 0)
            def _():
                total[...] = product

            @pl.when(start > 0)
            def _():
                total[...] += product

        left = pieces % DEEP

        @pl.when(lax.rem(p, DEEP) == DEEP - 1)
        def _():
            some(DEEP)

        if left:

            @pl.when(p == pieces - 1)
            def _():
                some(left)

        @pl.when(p == pieces - 1)
        def _():
            rs_own[pb] = total[c]
            rs_out[pb] = total[...].astype(jnp.bfloat16)
            for k in range(1, C):
                reduce_copy(pb, k).start()
            for d in range(2):

                @pl.when((place[d] < R - 1) & squares_went(d, pb))
                def _():
                    square_copy(d, pb).wait_send()

    def reduce(i, phase, block, p):
        @pl.when(p == pieces - 1)
        def _():
            pb = phase * blocks + block
            branch = rs_own[pb]
            for k in range(1, C):
                reduce_copy(pb, k).wait_recv()
                branch = branch + rs_in[pb, k - 1].astype(jnp.float32)

            @pl.when(phase == 0)
            def _():
                values = stream_in[block, c].astype(jnp.float32)
                merged[pb, c] = (values + 0.5 * branch).astype(jnp.bfloat16)

            @pl.when(phase == 1)
            def _():
                values = merged[block, c].astype(jnp.float32)
                merged[pb, c] = (values + 0.5 * branch).astype(jnp.bfloat16)

            for k in range(1, C):
                spread_copy(pb, k).start()

            @pl.when(pb > 0)
            def _():
                for k in range(1, C):
                    reduce_copy(pb - 1, k).wait_send()
                    spread_copy(pb - 1, k).wait_send()

    def spread(i, phase, block, p):
        @pl.when(p == pieces - 1)
        def _():
            pb = phase * blocks + block
            for k in range(1, C):
                spread_copy(pb, k).wait_recv()

            @pl.when(phase == 0)
            def _():
                normed[block], square = scaled(merged[pb].reshape(rows, -1), gain_second)
                keep_square(1, block, square)

            @pl.when(phase == 1)
            def _():
                out_copy(block).start()

    reach = HOP * (R - 1)
    end = 2 * reach

    def step(s, carry):
        load_rest(s)
        for d in range(2):
            at_step(s - 1 - HOP * place[d], forward(d), d)
        for d in range(2):
            at_step(s - 1 - reach - HOP * (R - 1 - place[d]), pass_back(d), d)
        at_step(s - 1 - end, down)
        at_step(s - 1 - end - REDUCE, reduce)
        at_step(s - 1 - end - REDUCE - SPREAD, spread)

        project_one(s)
        project_two(s)
        return carry

    lax.fori_loop(0, count + gap + end + REDUCE + SPREAD + 1, step, 0)

    for i in range(max(0, count - 2 * BEHIND), count):
        d = i % 2

        @pl.when(place[d] < R - 1)
        def _(d=d, i=i):
            part_copy(d, i).wait_send()

        @pl.when(place[d] > 0)
        def _(d=d, i=i):
            hidden_copy(d, i).wait_send()

    for k in range(1, C):
        reduce_copy(2 * blocks - 1, k).wait_send()
        spread_copy(2 * blocks - 1, k).wait_send()
    for block in range(blocks):
        out_copy(block).wait()


def solution(mesh):
    R, C = mesh.shape["ra"], mesh.shape["cb"]

    def per_device(
        residual,
        gain_first,
        gate_first,
        up_first,
        down_first,
        gain_second,
        gate_second,
        up_second,
        down_second,
    ):
        tokens, depth = residual.shape
        units = gate_first.shape[1]
        blocks = max(1, min(4, tokens // (16 * C)))
        width = 2 * LANES if units % (2 * LANES) == 0 else units
        pieces = units // width
        rows = tokens // blocks
        share = rows // C
        count = 2 * blocks * pieces
        end = 1 + 2 * HOP * (R - 1) + REDUCE + SPREAD
        gap = max(0, pieces - 1 + end - blocks * pieces)
        bf16, f32 = jnp.bfloat16, jnp.float32
        vmem = functools.partial(pl.BlockSpec, memory_space=pltpu.VMEM)
        hbm = functools.partial(pl.BlockSpec, memory_space=pl.ANY)
        pbs = 2 * blocks
        dma = pltpu.SemaphoreType.DMA
        result = pl.pallas_call(
            functools.partial(
                kernel, (R, C, blocks, pieces, width, rows, gap, float(depth * R))
            ),
            out_shape=jax.ShapeDtypeStruct((blocks, C, share, depth), bf16),
            in_specs=[hbm()] + [vmem()] * 2 + [hbm()] * 6,
            out_specs=hbm(),
            scratch_shapes=[
                pltpu.VMEM((2, pieces, 2, depth, width), bf16),
                pltpu.VMEM((2, pieces, width, depth), bf16),
                pltpu.VMEM((blocks, C, share, depth), bf16),
                pltpu.VMEM((tokens, depth), bf16),
                pltpu.VMEM((blocks, rows, depth), bf16),
                pltpu.VMEM((blocks * pieces, 2, rows, width), f32),
                pltpu.VMEM((count, 2, rows, width), bf16),
                pltpu.VMEM((count, 2, rows, width), bf16),
                pltpu.VMEM((count, rows, width), bf16),
                pltpu.VMEM((C, share, depth), f32),
                pltpu.VMEM((pbs, share, depth), f32),
                pltpu.VMEM((pbs, C, share, depth), bf16),
                pltpu.VMEM((pbs, C - 1, share, depth), bf16),
                pltpu.VMEM((pbs, C, share, depth), bf16),
                pltpu.VMEM((2, blocks, TILE, rows), f32),
                pltpu.VMEM((pbs, 2, TILE, rows), f32),
                pltpu.VMEM((pbs, 2, TILE, rows), f32),
                pltpu.VMEM((2, rows, LANES), f32),
                dma((2, 3, pieces)),
                dma,
                dma((blocks,)),
                dma((count,)),
                dma((count,)),
                dma((count,)),
                dma((count,)),
                dma((2, pbs)),
                dma((2, pbs)),
                dma((pbs, C - 1)),
                dma((pbs, C - 1)),
                dma((pbs, C - 1)),
                dma((pbs, C - 1)),
            ],
            compiler_params=pltpu.CompilerParams(
                collective_id=0, has_side_effects=True, vmem_limit_bytes=67043328
            ),
        )(
            residual.reshape(blocks, C, share, depth),
            gain_first,
            gain_second,
            gate_first,
            up_first,
            down_first,
            gate_second,
            up_second,
            down_second,
        )
        return result.reshape(tokens, depth)

    in_specs = (
        P("grp", "ra"),
        P("ra"),
        P("ra", "cb"),
        P("ra", "cb"),
        P("cb", "ra"),
        P("ra"),
        P("ra", "cb"),
        P("ra", "cb"),
        P("cb", "ra"),
    )
    return jax.shard_map(
        per_device, mesh=mesh, in_specs=in_specs, out_specs=P("grp", "ra"), check_vma=False
    )
```

```python
import functools
import heapq

import jax
import jax.numpy as jnp
from jax import lax
from jax.experimental import pallas as pl
from jax.experimental.pallas import tpu as pltpu
from jax.sharding import PartitionSpec as P

MESH = pl.DeviceIdType.MESH
LANES = 128
epsilon = 1e-06

TILE = 8
AHEAD = 3
BEHIND = 4
WIDE = 1
DEEP = 3
UNIT = 1.405

FORWARD, BACKWARD, DOWN, PAIR, ACROSS, SETTLE, PROJECT_ONE, PROJECT_TWO, REST = 0, 2, 4, 5, 6, 7, 8, 9, 10
COST = {
    "op": 0.12, "forward": 0.1, "finish": 0.16, "backward": 0.02, "down": 0.16, "project_one": 0.45,
    "project_two": 0.3, "pair": 0.1, "across": 0.1, "settle": 0.2, "hop": 2.2, "near": 1.8, "far": 4.2,
    "queue": 2.0, "bubble": 0.05,
}
RANK = {
    "settle": 0.5, "across": 0.6, "pair": 0.7, "backward0": 2, "forward1": 2.5, "forward0": 3,
    "project_one": 3.6, "down0": 4, "backward1": 4.75, "project_two": 5.2, "down1": 6.4,
}


def plan(R, blocks, pieces, deep, wide, busy, cost=COST, rank=RANK):
    per_phase = blocks * pieces
    count = 2 * per_phase
    heap = []
    ticket = 0
    groups = []
    for pb in range(2 * blocks):
        for start in range(0, pieces, deep):
            groups.append((pb, start, min(deep, pieces - start)))
    wides = []
    for block in range(blocks):
        for start in range(0, pieces, wide):
            wides.append((block, start, min(wide, pieces - start)))
    units = [[i for i in range(count) if i % 2 == d] for d in range(2)]
    nodes = []
    for z in range(R):
        nodes.append(dict(
            time=0.0, own=set(), forward=[0, 0], backward=[0, 0], down=0, pair=0, across=0, settle=0,
            one=0, two=0, sums=set(), hidden=set(), done=set(), near={}, far={}, back={}, order=[],
        ))
    free = {}
    sent = {}

    def poke(time, z):
        nonlocal ticket
        ticket += 1
        heapq.heappush(heap, (time, ticket, "try", z, None))

    def land(time, z, where, key):
        nonlocal ticket
        ticket += 1
        heapq.heappush(heap, (time, ticket, where, z, key))

    for z in range(R):
        poke(0.0, z)
        for p in range(pieces):
            poke(0.3 * (p + 1), z)
    while heap:
        now, _, event, z, key = heapq.heappop(heap)
        node = nodes[z]
        if event != "try":
            if event in ("sums", "hidden"):
                node[event].add(key)
            else:
                node[event][key] = now
        if node["time"] > now + 1e-9:
            continue
        place = (z, R - 1 - z)
        best = None

        def offer(name, kind, value, duration):
            nonlocal best
            if best is None or rank[name] < best[0]:
                best = (rank[name], kind, value, duration)

        wake = []

        def open_link(way):
            until = free.get((z, way), 0.0) - cost["queue"]
            if until > now + 1e-9:
                wake.append(until)
                return False
            return True

        for d in range(2):
            way = 1 - 2 * d
            at = node["forward"][d]
            if at < len(units[d]):
                i = units[d][at]
                if i in node["own"] and (place[d] == 0 or i in node["sums"]):
                    phase = i // per_phase
                    if place[d] == R - 1:
                        offer("forward%d" % phase, FORWARD, i, cost["finish"])
                    elif open_link(way):
                        offer("forward%d" % phase, FORWARD, i, cost["forward"])
            at = node["backward"][d]
            if place[d] > 0 and at < len(units[d]):
                i = units[d][at]
                if i in (node["done"] if place[d] == R - 1 else node["hidden"]) and open_link(-way):
                    offer("backward%d" % (i // per_phase), BACKWARD, i, cost["backward"])
        if node["down"] < len(groups):
            pb, start, size = groups[node["down"]]
            ready = True
            for i in range(pb * pieces + start, pb * pieces + start + size):
                d = i % 2
                if place[d] == 0:
                    ready &= i in node["hidden"]
                elif place[d] == R - 1:
                    ready &= i in node["done"]
                else:
                    ready &= units[d].index(i) < node["backward"][d]
            if ready:
                offer("down%d" % (pb // blocks), DOWN, node["down"], cost["down"] * size)
        for name, kind, source in (("pair", PAIR, "near"), ("across", ACROSS, "far"), ("settle", SETTLE, "back")):
            if node[source].get(node[name], 1e9) <= now + 1e-9:
                offer(name, kind, node[name], cost[name])
        if node["one"] < pieces and 0.3 * (node["one"] + 1) <= now + 1e-9:
            offer("project_one", PROJECT_ONE, node["one"], cost["project_one"])
        if node["two"] < len(wides):
            block, start, size = wides[node["two"]]
            if node["settle"] > block:
                offer("project_two", PROJECT_TWO, block * pieces + start, cost["project_two"] * size)
        if best is None:
            for until in wake:
                poke(until, z)
            continue
        _, kind, value, duration = best
        node["order"].append(kind + value % 2 if kind in (FORWARD, BACKWARD) else kind)
        end = now + cost["op"] + duration
        node["time"] = end

        def send(way, size, where, i):
            begin = max(end, free.get((z, way), 0.0))
            free[(z, way)] = begin + size + cost["bubble"]
            land(free[(z, way)] + cost["hop"], z + way, where, i)

        if kind in (FORWARD, BACKWARD):
            d = value % 2
            way = 1 - 2 * d
            if kind == FORWARD:
                node["forward"][d] += 1
                if place[d] == R - 1:
                    node["done"].add(value)
                else:
                    send(way, busy, "sums", value)
            else:
                node["backward"][d] += 1
                send(-way, busy / 2, "hidden", value)
        elif kind == DOWN:
            pb, start, size = groups[value]
            node["down"] += 1
            if start + size == pieces:
                land(end + cost["near"], z, "near", pb)
        elif kind == PAIR:
            node["pair"] += 1
            land(end + cost["far"], z, "far", value)
        elif kind == ACROSS:
            node["across"] += 1
            land(end + cost["near"], z, "back", value)
        elif kind == SETTLE:
            node["settle"] += 1
        elif kind == PROJECT_ONE:
            node["one"] += 1
            node["own"].update(block * pieces + value for block in range(blocks))
        else:
            block, start, size = wides[node["two"]]
            node["two"] += 1
            node["own"].update(per_phase + value + q for q in range(size))
        poke(end, z)
    for node in nodes:
        assert node["settle"] == 2 * blocks
    orders = [node["order"] for node in nodes]
    return orders


def kernel(
    cfg,
    residual,
    gain_first,
    gain_second,
    gate_first,
    up_first,
    down_first,
    gate_second,
    up_second,
    down_second,
    out,
    w_in,
    w_down,
    stream_in,
    normed_one,
    normed,
    own,
    part_out,
    part_in,
    hidden,
    total,
    table,
    pair_own,
    pair_out,
    pair_in,
    shares,
    merged,
    sq_own,
    sq_out,
    sq_in,
    scale,
    w_sem,
    x_sem,
    part_send,
    part_recv,
    hid_send,
    hid_recv,
    sq_send,
    sq_recv,
    pair_send,
    pair_recv,
    rs_send,
    rs_recv,
    ag_send,
    ag_recv,
):
    R, C, blocks, pieces, width, rows, orders, model = cfg
    per_phase = blocks * pieces
    count = 2 * per_phase
    r = lax.axis_index("ra")
    c = lax.axis_index("cb")
    X = C // 2
    side, spot = lax.rem(c, 2), lax.div(c, 2)
    half = rows // 2
    length = max(len(order) for order in orders)

    gates, ups, downs = (gate_first, gate_second), (up_first, up_second), (down_first, down_second)

    def weight_copy(phase, p, which):
        span = pl.ds(p * width if pieces > 1 else 0, width)
        if which == 2:
            return pltpu.make_async_copy(
                downs[phase].at[span, :], w_down.at[phase, p], w_sem.at[phase, 2, p]
            )
        source = (gates, ups)[which][phase]
        return pltpu.make_async_copy(
            source.at[:, span], w_in.at[phase, p, which], w_sem.at[phase, which, p]
        )

    stream_copy = pltpu.make_async_copy(residual, stream_in, x_sem)
    stream_copy.start()
    for p in range(min(AHEAD, pieces)):
        weight_copy(0, p, 0).start()
        weight_copy(0, p, 1).start()

    for z, order in enumerate(orders):

        @pl.when(r == z)
        def _(order=order):
            for at, kind in enumerate(order):
                table[at] = kind
            for at in range(len(order), length):
                table[at] = REST

    barrier = pltpu.get_barrier_semaphore()

    @pl.when(r > 0)
    def _():
        pl.semaphore_signal(barrier, inc=1, device_id={"ra": r - 1}, device_id_type=MESH)

    @pl.when(r < R - 1)
    def _():
        pl.semaphore_signal(barrier, inc=1, device_id={"ra": r + 1}, device_id_type=MESH)

    for k in range(1, C):
        pl.semaphore_signal(
            barrier, inc=1, device_id={"cb": lax.rem(c + k, C)}, device_id_type=MESH
        )

    def diagonal():
        shape = (rows, rows)
        return lax.broadcasted_iota(jnp.int32, shape, 0) == lax.broadcasted_iota(jnp.int32, shape, 1)

    def scaled(stream, gain_ref):
        values = stream.astype(jnp.float32)
        square = jnp.sum(values * values, axis=1, keepdims=True)
        gain = gain_ref[...].astype(jnp.float32).reshape(1, -1)
        return (values * gain).astype(jnp.bfloat16), square

    def keep_square(phase, block, square):
        line = jnp.sum(jnp.where(diagonal(), square, 0.0), axis=0, keepdims=True)
        sq_own[phase, block] = jnp.broadcast_to(line, (TILE, rows))

    stream_copy.wait()
    for block in range(blocks):
        normed_one[pl.ds(block * rows, rows)], square = scaled(
            stream_in[block].reshape(rows, -1), gain_first
        )
        keep_square(0, block, square)

    near = jnp.where(r > 0, 1, 0) + jnp.where(r < R - 1, 1, 0)
    pl.semaphore_wait(barrier, C - 1 + near)

    def of_side(d):
        rise = d == 0
        place = jnp.where(rise, r, R - 1 - r)
        return place, jnp.where(rise, r + 1, r - 1), jnp.where(rise, r - 1, r + 1)

    def part_copy(i):
        return pltpu.make_async_remote_copy(
            src_ref=part_out.at[i],
            dst_ref=part_in.at[i],
            send_sem=part_send.at[i],
            recv_sem=part_recv.at[i],
            device_id={"ra": of_side(lax.rem(i, 2))[1]},
            device_id_type=MESH,
        )

    def square_copy(d, pb):
        return pltpu.make_async_remote_copy(
            src_ref=sq_out.at[pb, d],
            dst_ref=sq_in.at[pb, d],
            send_sem=sq_send.at[d, pb],
            recv_sem=sq_recv.at[d, pb],
            device_id={"ra": of_side(d)[1]},
            device_id_type=MESH,
        )

    def hidden_copy(i):
        return pltpu.make_async_remote_copy(
            src_ref=hidden.at[i],
            dst_ref=hidden.at[i],
            send_sem=hid_send.at[i],
            recv_sem=hid_recv.at[i],
            device_id={"ra": of_side(lax.rem(i, 2))[2]},
            device_id_type=MESH,
        )

    def squares_went(d, pb):
        return (pieces > 1) | (lax.rem(pb, 2) == d)

    def pair_copy(pb):
        return pltpu.make_async_remote_copy(
            src_ref=pair_out.at[pb],
            dst_ref=pair_in.at[pb],
            send_sem=pair_send.at[pb],
            recv_sem=pair_recv.at[pb],
            device_id={"cb": c + 1 - 2 * side},
            device_id_type=MESH,
        )

    def across_copy(pb, k):
        return pltpu.make_async_remote_copy(
            src_ref=shares.at[pb, spot],
            dst_ref=shares.at[pb, spot],
            send_sem=rs_send.at[pb, k - 1],
            recv_sem=rs_recv.at[pb, k - 1],
            device_id={"cb": 2 * lax.rem(spot + k, X) + side},
            device_id_type=MESH,
        )

    def spread_copy(pb):
        return pltpu.make_async_remote_copy(
            src_ref=merged.at[pb, side],
            dst_ref=merged.at[pb, side],
            send_sem=ag_send.at[pb],
            recv_sem=ag_recv.at[pb],
            device_id={"cb": c + 1 - 2 * side},
            device_id_type=MESH,
        )

    def unit_of(i):
        phase = jnp.where(i >= per_phase, 1, 0)
        local = i - phase * per_phase
        return phase, lax.div(local, pieces), lax.rem(local, pieces)

    def project_one(p):
        @pl.when(p + AHEAD < pieces)
        def _():
            weight_copy(0, p + AHEAD, 0).start()
            weight_copy(0, p + AHEAD, 1).start()

        weight_copy(0, p, 2).start()
        for which in range(2):
            weight_copy(0, p, which).wait()
        x = normed_one[...]
        for which in range(2):
            product = jnp.dot(x, w_in[0, p, which], preferred_element_type=jnp.float32)
            for block in range(blocks):
                own[block * pieces + p, which] = product[block * rows : (block + 1) * rows]

    def grouped(p, size, body):
        left = pieces % size
        if left == 0:
            body(size)
        elif left == pieces:
            body(left)
        else:

            @pl.when(p + size <= pieces)
            def _():
                body(size)

            @pl.when(p + size > pieces)
            def _():
                body(left)

    def project_two(local):
        block = lax.div(local, pieces)
        p = lax.rem(local, pieces)

        def some(size):
            @pl.when(block == 0)
            def _():
                for q in range(size):
                    weight_copy(1, p + q, 0).wait()
                    weight_copy(1, p + q, 1).wait()

            x = normed[block]
            for q in range(size):
                for which in range(2):
                    own[local + q, which] = jnp.dot(
                        x, w_in[1, p + q, which], preferred_element_type=jnp.float32
                    )

        grouped(p, WIDE, some)

    def forward(i, d):
        phase, block, p = unit_of(i)
        place = of_side(d)[0]
        slot = i - phase * per_phase
        pb = phase * blocks + block
        opening = p < 2
        old = i - 2 * BEHIND

        @pl.when((place < R - 1) & (old >= 0))
        def _():
            part_copy(old).wait_send()

        @pl.when(place == 0)
        def _():
            part_out[i] = own[slot].astype(jnp.bfloat16)
            part_copy(i).start()

            @pl.when(opening)
            def _():
                sq_out[pb, d] = sq_own[phase, block]
                square_copy(d, pb).start()

        @pl.when((place > 0) & (place < R - 1))
        def _():
            part_copy(i).wait_recv()
            part_out[i] = (own[slot] + part_in[i].astype(jnp.float32)).astype(jnp.bfloat16)
            part_copy(i).start()

            @pl.when(opening)
            def _():
                square_copy(d, pb).wait_recv()
                sq_out[pb, d] = sq_own[phase, block] + sq_in[pb, d]
                square_copy(d, pb).start()

        @pl.when(place == R - 1)
        def _():
            @pl.when(opening)
            def _():
                square_copy(d, pb).wait_recv()
                mean = (sq_own[phase, block] + sq_in[pb, d])[:1] / model
                line = lax.rsqrt(mean + epsilon)
                column = jnp.sum(jnp.where(diagonal(), line, 0.0), axis=1, keepdims=True)
                scale[d] = jnp.broadcast_to(column, (rows, LANES))

            part_copy(i).wait_recv()
            factor = scale[d][:, :1]
            gate = (own[slot, 0] + part_in[i, 0].astype(jnp.float32)) * factor
            up = (own[slot, 1] + part_in[i, 1].astype(jnp.float32)) * factor
            hidden[i] = (gate / (1.0 + jnp.exp(-gate)) * up).astype(jnp.bfloat16)

    def backward(i, d):
        place = of_side(d)[0]

        @pl.when(place < R - 1)
        def _():
            hidden_copy(i).wait_recv()

        hidden_copy(i).start()

        @pl.when(i >= 2 * BEHIND)
        def _():
            hidden_copy(i - 2 * BEHIND).wait_send()

    steps = -(-pieces // DEEP)

    def down(group):
        pb = lax.div(group, steps)
        phase = jnp.where(pb >= blocks, 1, 0)
        start = lax.rem(group, steps) * DEEP

        def some(size):
            for q in range(size):
                i = pb * pieces + start + q

                @pl.when(of_side(lax.rem(i, 2))[0] == 0)
                def _(i=i):
                    hidden_copy(i).wait_recv()

                @pl.when(pb == 0)
                def _(q=q):
                    weight_copy(0, start + q, 2).wait()
                    weight_copy(1, start + q, 0).start()
                    weight_copy(1, start + q, 1).start()
                    weight_copy(1, start + q, 2).start()

                @pl.when(pb == blocks)
                def _(q=q):
                    weight_copy(1, start + q, 2).wait()

            slot = pb * pieces + start
            product = jnp.dot(
                jnp.concatenate([hidden[slot + q] for q in range(size)], axis=1),
                w_down[phase, pl.ds(start, size)].reshape(size * width, -1),
                preferred_element_type=jnp.float32,
            )

            @pl.when(start == 0)
            def _():
                total[...] = product.reshape(total.shape)

            @pl.when(start > 0)
            def _():
                total[...] += product.reshape(total.shape)

        grouped(start, DEEP, some)

        @pl.when(start + DEEP >= pieces)
        def _():
            pair_own[lax.rem(pb, 2)] = total[side]
            pair_out[pb] = total[1 - side]
            pair_copy(pb).start()
            for d in range(2):

                @pl.when((of_side(d)[0] < R - 1) & squares_went(d, pb))
                def _(d=d):
                    square_copy(d, pb).wait_send()

    def pair(pb):
        pair_copy(pb).wait_recv()
        shares[pb, spot] = (pair_own[lax.rem(pb, 2)] + pair_in[pb]).astype(jnp.bfloat16)
        for k in range(1, X):
            across_copy(pb, k).start()

        @pl.when(pb > 0)
        def _():
            pair_copy(pb - 1).wait_send()

    def across(pb):
        for k in range(1, X):
            across_copy(pb, k).wait_recv()
        branch = shares[pb, 0].astype(jnp.float32)
        for x in range(1, X):
            branch = branch + shares[pb, x].astype(jnp.float32)

        @pl.when(pb < blocks)
        def _():
            values = stream_in[pb, side].astype(jnp.float32)
            merged[pb, side] = (values + 0.5 * branch).astype(jnp.bfloat16)

        @pl.when(pb >= blocks)
        def _():
            values = merged[pb - blocks, side].astype(jnp.float32)
            merged[pb, side] = (values + 0.5 * branch).astype(jnp.bfloat16)

        spread_copy(pb).start()

        @pl.when(pb > 0)
        def _():
            for k in range(1, X):
                across_copy(pb - 1, k).wait_send()
            spread_copy(pb - 1).wait_send()

    def settle(pb):
        spread_copy(pb).wait_recv()

        @pl.when(pb < blocks)
        def _():
            normed[pb], square = scaled(merged[pb].reshape(rows, -1), gain_second)
            keep_square(1, pb, square)

        @pl.when(pb >= blocks)
        def _():
            out[pb - blocks] = merged[pb]

    bodies = (
        lambda n: forward(2 * n, 0),
        lambda n: forward(2 * n + 1, 1),
        lambda n: backward(2 * n, 0),
        lambda n: backward(2 * n + 1, 1),
        down,
        pair,
        across,
        settle,
        project_one,
        project_two,
    )

    def step(at, counts):
        what = table[at]

        def one(kind):
            def run():
                bodies[kind](counts[kind])
                return counts[kind] + 1

            return lax.cond(what == kind, run, lambda: counts[kind])

        return tuple(one(kind) for kind in range(len(bodies)))

    lax.fori_loop(0, length, step, (jnp.int32(0),) * len(bodies))

    for i in range(max(0, count - 2 * BEHIND), count):
        place = of_side(i % 2)[0]

        @pl.when(place < R - 1)
        def _(i=i):
            part_copy(i).wait_send()

        @pl.when(place > 0)
        def _(i=i):
            hidden_copy(i).wait_send()

    newest = 2 * blocks - 1
    pair_copy(newest).wait_send()
    for k in range(1, X):
        across_copy(newest, k).wait_send()
    spread_copy(newest).wait_send()


def solution(mesh):
    R, C = mesh.shape["ra"], mesh.shape["cb"]

    def per_device(
        residual,
        gain_first,
        gate_first,
        up_first,
        down_first,
        gain_second,
        gate_second,
        up_second,
        down_second,
    ):
        tokens, depth = residual.shape
        units = gate_first.shape[1]
        blocks = max(1, min(4, tokens // (16 * C)))
        width = 2 * LANES if units % (2 * LANES) == 0 else units
        pieces = units // width
        rows = tokens // blocks
        count = 2 * blocks * pieces
        half = rows // 2
        orders = plan(R, blocks, pieces, DEEP, WIDE, UNIT)
        length = max(len(order) for order in orders)
        bf16, f32 = jnp.bfloat16, jnp.float32
        vmem = functools.partial(pl.BlockSpec, memory_space=pltpu.VMEM)
        hbm = functools.partial(pl.BlockSpec, memory_space=pl.ANY)
        pbs = 2 * blocks
        dma = pltpu.SemaphoreType.DMA
        result = pl.pallas_call(
            functools.partial(
                kernel, (R, C, blocks, pieces, width, rows, orders, float(depth * R))
            ),
            out_shape=pltpu.VMEM((blocks, 2, half, depth), bf16),
            in_specs=[hbm()] + [vmem()] * 2 + [hbm()] * 6,
            out_specs=vmem(),
            scratch_shapes=[
                pltpu.VMEM((2, pieces, 2, depth, width), bf16),
                pltpu.VMEM((2, pieces, width, depth), bf16),
                pltpu.VMEM((blocks, 2, half, depth), bf16),
                pltpu.VMEM((tokens, depth), bf16),
                pltpu.VMEM((blocks, rows, depth), bf16),
                pltpu.VMEM((blocks * pieces, 2, rows, width), f32),
                pltpu.VMEM((count, 2, rows, width), bf16),
                pltpu.VMEM((count, 2, rows, width), bf16),
                pltpu.VMEM((count, rows, width), bf16),
                pltpu.VMEM((2, half, depth), f32),
                pltpu.SMEM((length,), jnp.int32),
                pltpu.VMEM((2, half, depth), f32),
                pltpu.VMEM((pbs, half, depth), f32),
                pltpu.VMEM((pbs, half, depth), f32),
                pltpu.VMEM((pbs, C // 2, half, depth), bf16),
                pltpu.VMEM((pbs, 2, half, depth), bf16),
                pltpu.VMEM((2, blocks, TILE, rows), f32),
                pltpu.VMEM((pbs, 2, TILE, rows), f32),
                pltpu.VMEM((pbs, 2, TILE, rows), f32),
                pltpu.VMEM((2, rows, LANES), f32),
                dma((2, 3, pieces)),
                dma,
                dma((count,)),
                dma((count,)),
                dma((count,)),
                dma((count,)),
                dma((2, pbs)),
                dma((2, pbs)),
                dma((pbs,)),
                dma((pbs,)),
                dma((pbs, max(1, C // 2 - 1))),
                dma((pbs, max(1, C // 2 - 1))),
                dma((pbs,)),
                dma((pbs,)),
            ],
            compiler_params=pltpu.CompilerParams(
                collective_id=0, has_side_effects=True, vmem_limit_bytes=66400000
            ),
        )(
            residual.reshape(blocks, 2, half, depth),
            gain_first,
            gain_second,
            gate_first,
            up_first,
            down_first,
            gate_second,
            up_second,
            down_second,
        )
        return result.reshape(tokens, depth)

    in_specs = (
        P("grp", "ra"),
        P("ra"),
        P("ra", "cb"),
        P("ra", "cb"),
        P("cb", "ra"),
        P("ra"),
        P("ra", "cb"),
        P("ra", "cb"),
        P("cb", "ra"),
    )
    return jax.shard_map(
        per_device, mesh=mesh, in_specs=in_specs, out_specs=P("grp", "ra"), check_vma=False
    )
```

```python
import functools
import heapq

import jax
import jax.numpy as jnp
from jax import lax
from jax.experimental import pallas as pl
from jax.experimental.pallas import tpu as pltpu
from jax.sharding import PartitionSpec as P

MESH = pl.DeviceIdType.MESH
LANES = 128
epsilon = 1e-06

TILE = 8
AHEAD = 3
BEHIND = 4
WIDE = 1
FIRST = 2
DEEP = 4
UNIT = 1.405

FORWARD, BACKWARD, DOWN, PAIR, ACROSS, SETTLE, PROJECT_ONE, PROJECT_TWO, REST = 0, 2, 4, 5, 6, 7, 8, 9, 10
COST = {
    "op": 0.12, "forward": 0.1, "finish": 0.16, "backward": 0.02, "down": 0.16, "project_one": 0.45,
    "project_two": 0.3, "pair": 0.1, "across": 0.1, "settle": 0.2, "hop": 2.2, "near": 1.8, "far": 4.2,
    "queue": 2.0, "bubble": 0.05,
}
RANK = {
    "settle": 0.5, "across": 0.6, "pair": 0.7, "backward0": 2, "forward1": 2.5, "forward0": 3,
    "project_one": 3.6, "down0": 4, "backward1": 4.75, "project_two": 5.2, "down1": 6.4,
}


def plan(R, blocks, pieces, deep, wide, busy, cost=COST, rank=RANK):
    per_phase = blocks * pieces
    count = 2 * per_phase
    heap = []
    ticket = 0
    groups = []
    for pb in range(2 * blocks):
        for start in range(0, pieces, deep):
            groups.append((pb, start, min(deep, pieces - start)))
    wides = []
    for block in range(blocks):
        for start in range(0, pieces, wide):
            wides.append((block, start, min(wide, pieces - start)))
    units = [[i for i in range(count) if i % 2 == d] for d in range(2)]
    nodes = []
    for z in range(R):
        nodes.append(dict(
            time=0.0, own={b * pieces + p for b in range(blocks) for p in range(min(FIRST, pieces))}, forward=[0, 0], backward=[0, 0], down=0, pair=0, across=0, settle=0,
            one=min(FIRST, pieces), two=0, sums=set(), hidden=set(), done=set(), near={}, far={}, back={}, order=[],
        ))
    free = {}
    sent = {}

    def poke(time, z):
        nonlocal ticket
        ticket += 1
        heapq.heappush(heap, (time, ticket, "try", z, None))

    def land(time, z, where, key):
        nonlocal ticket
        ticket += 1
        heapq.heappush(heap, (time, ticket, where, z, key))

    for z in range(R):
        poke(0.0, z)
        for p in range(pieces):
            poke(0.3 * (p + 1), z)
    while heap:
        now, _, event, z, key = heapq.heappop(heap)
        node = nodes[z]
        if event != "try":
            if event in ("sums", "hidden"):
                node[event].add(key)
            else:
                node[event][key] = now
        if node["time"] > now + 1e-9:
            continue
        place = (z, R - 1 - z)
        best = None

        def offer(name, kind, value, duration):
            nonlocal best
            if best is None or rank[name] < best[0]:
                best = (rank[name], kind, value, duration)

        wake = []

        def open_link(way):
            until = free.get((z, way), 0.0) - cost["queue"]
            if until > now + 1e-9:
                wake.append(until)
                return False
            return True

        for d in range(2):
            way = 1 - 2 * d
            at = node["forward"][d]
            if at < len(units[d]):
                i = units[d][at]
                if i in node["own"] and (place[d] == 0 or i in node["sums"]):
                    phase = i // per_phase
                    if place[d] == R - 1:
                        offer("forward%d" % phase, FORWARD, i, cost["finish"])
                    elif open_link(way):
                        offer("forward%d" % phase, FORWARD, i, cost["forward"])
            at = node["backward"][d]
            if place[d] > 0 and at < len(units[d]):
                i = units[d][at]
                if i in (node["done"] if place[d] == R - 1 else node["hidden"]) and open_link(-way):
                    offer("backward%d" % (i // per_phase), BACKWARD, i, cost["backward"])
        if node["down"] < len(groups):
            pb, start, size = groups[node["down"]]
            ready = True
            for i in range(pb * pieces + start, pb * pieces + start + size):
                d = i % 2
                if place[d] == 0:
                    ready &= i in node["hidden"]
                elif place[d] == R - 1:
                    ready &= i in node["done"]
                else:
                    ready &= units[d].index(i) < node["backward"][d]
            if ready:
                offer("down%d" % (pb // blocks), DOWN, node["down"], cost["down"] * size)
        for name, kind, source in (("pair", PAIR, "near"), ("across", ACROSS, "far"), ("settle", SETTLE, "back")):
            if node[source].get(node[name], 1e9) <= now + 1e-9:
                offer(name, kind, node[name], cost[name])
        if node["one"] < pieces and 0.3 * (node["one"] + 1) <= now + 1e-9:
            offer("project_one", PROJECT_ONE, node["one"], cost["project_one"])
        if node["two"] < len(wides):
            block, start, size = wides[node["two"]]
            if node["settle"] > block:
                offer("project_two", PROJECT_TWO, block * pieces + start, cost["project_two"] * size)
        if best is None:
            for until in wake:
                poke(until, z)
            continue
        _, kind, value, duration = best
        node["order"].append(kind + value % 2 if kind in (FORWARD, BACKWARD) else kind)
        end = now + cost["op"] + duration
        node["time"] = end

        def send(way, size, where, i):
            begin = max(end, free.get((z, way), 0.0))
            free[(z, way)] = begin + size + cost["bubble"]
            land(free[(z, way)] + cost["hop"], z + way, where, i)

        if kind in (FORWARD, BACKWARD):
            d = value % 2
            way = 1 - 2 * d
            if kind == FORWARD:
                node["forward"][d] += 1
                if place[d] == R - 1:
                    node["done"].add(value)
                else:
                    send(way, busy, "sums", value)
            else:
                node["backward"][d] += 1
                send(-way, busy / 2, "hidden", value)
        elif kind == DOWN:
            pb, start, size = groups[value]
            node["down"] += 1
            if start + size == pieces:
                land(end + cost["near"], z, "near", pb)
        elif kind == PAIR:
            node["pair"] += 1
            land(end + cost["far"], z, "far", value)
        elif kind == ACROSS:
            node["across"] += 1
            land(end + cost["near"], z, "back", value)
        elif kind == SETTLE:
            node["settle"] += 1
        elif kind == PROJECT_ONE:
            node["one"] += 1
            node["own"].update(block * pieces + value for block in range(blocks))
        else:
            block, start, size = wides[node["two"]]
            node["two"] += 1
            node["own"].update(per_phase + value + q for q in range(size))
        poke(end, z)
    for node in nodes:
        assert node["settle"] == 2 * blocks
    orders = [node["order"] for node in nodes]
    return orders


def kernel(
    cfg,
    residual,
    gain_first,
    gain_second,
    gate_first,
    up_first,
    down_first,
    gate_second,
    up_second,
    down_second,
    out,
    w_in,
    w_down,
    stream_in,
    gain_one,
    gain_two,
    normed_one,
    normed,
    own,
    part_out,
    part_in,
    hidden,
    total,
    table,
    pair_own,
    pair_out,
    pair_in,
    shares,
    merged,
    sq_own,
    sq_out,
    sq_in,
    scale,
    w_sem,
    x_sem,
    gain_sem,
    part_send,
    part_recv,
    hid_send,
    hid_recv,
    sq_send,
    sq_recv,
    pair_send,
    pair_recv,
    rs_send,
    rs_recv,
    ag_send,
    ag_recv,
):
    R, C, blocks, pieces, width, rows, orders, model = cfg
    per_phase = blocks * pieces
    count = 2 * per_phase
    r = lax.axis_index("ra")
    c = lax.axis_index("cb")
    X = C // 2
    side, spot = lax.rem(c, 2), lax.div(c, 2)
    half = rows // 2
    length = max(len(order) for order in orders)

    gates, ups, downs = (gate_first, gate_second), (up_first, up_second), (down_first, down_second)

    def weight_copy(phase, p, which):
        span = pl.ds(p * width if pieces > 1 else 0, width)
        if which == 2:
            return pltpu.make_async_copy(
                downs[phase].at[span, :], w_down.at[phase, p], w_sem.at[phase, 2, p]
            )
        source = (gates, ups)[which][phase]
        return pltpu.make_async_copy(
            source.at[:, span], w_in.at[phase, p, which], w_sem.at[phase, which, p]
        )

    stream_copy = pltpu.make_async_copy(residual, stream_in, x_sem)
    stream_copy.start()
    gain_copies = [
        pltpu.make_async_copy(source, kept, gain_sem.at[at])
        for at, (source, kept) in enumerate(((gain_first, gain_one), (gain_second, gain_two)))
    ]
    gain_copies[0].start()
    gain_copies[1].start()
    for p in range(min(AHEAD, pieces)):
        weight_copy(0, p, 0).start()
        weight_copy(0, p, 1).start()

    for z, order in enumerate(orders):

        @pl.when(r == z)
        def _(order=order):
            for at, kind in enumerate(order):
                table[at] = kind
            for at in range(len(order), length):
                table[at] = REST

    barrier = pltpu.get_barrier_semaphore()

    @pl.when(r > 0)
    def _():
        pl.semaphore_signal(barrier, inc=1, device_id={"ra": r - 1}, device_id_type=MESH)

    @pl.when(r < R - 1)
    def _():
        pl.semaphore_signal(barrier, inc=1, device_id={"ra": r + 1}, device_id_type=MESH)

    for k in range(1, C):
        pl.semaphore_signal(
            barrier, inc=1, device_id={"cb": lax.rem(c + k, C)}, device_id_type=MESH
        )

    def diagonal():
        shape = (rows, rows)
        return lax.broadcasted_iota(jnp.int32, shape, 0) == lax.broadcasted_iota(jnp.int32, shape, 1)

    def scaled(stream, gain_ref):
        values = stream.astype(jnp.float32)
        square = jnp.sum(values * values, axis=1, keepdims=True)
        gain = gain_ref[...].astype(jnp.float32).reshape(1, -1)
        return (values * gain).astype(jnp.bfloat16), square

    def keep_square(phase, block, square):
        line = jnp.sum(jnp.where(diagonal(), square, 0.0), axis=0, keepdims=True)
        sq_own[phase, block] = jnp.broadcast_to(line, (TILE, rows))

    stream_copy.wait()
    gain_copies[0].wait()
    gain_copies[1].wait()
    for block in range(blocks):
        normed_one[pl.ds(block * rows, rows)], square = scaled(
            stream_in[block].reshape(rows, -1), gain_one
        )
        keep_square(0, block, square)

    def project_one(p):
        @pl.when(p + AHEAD < pieces)
        def _():
            weight_copy(0, p + AHEAD, 0).start()
            weight_copy(0, p + AHEAD, 1).start()

        weight_copy(0, p, 2).start()
        for which in range(2):
            weight_copy(0, p, which).wait()
        x = normed_one[...]
        for which in range(2):
            product = jnp.dot(x, w_in[0, p, which], preferred_element_type=jnp.float32)
            for block in range(blocks):
                own[block * pieces + p, which] = product[block * rows : (block + 1) * rows]

    for p in range(min(FIRST, pieces)):
        project_one(p)

    near = jnp.where(r > 0, 1, 0) + jnp.where(r < R - 1, 1, 0)
    pl.semaphore_wait(barrier, C - 1 + near)

    def of_side(d):
        rise = d == 0
        place = jnp.where(rise, r, R - 1 - r)
        return place, jnp.where(rise, r + 1, r - 1), jnp.where(rise, r - 1, r + 1)

    def part_copy(i):
        return pltpu.make_async_remote_copy(
            src_ref=part_out.at[i],
            dst_ref=part_in.at[i],
            send_sem=part_send.at[i],
            recv_sem=part_recv.at[i],
            device_id={"ra": of_side(lax.rem(i, 2))[1]},
            device_id_type=MESH,
        )

    def square_copy(d, pb):
        return pltpu.make_async_remote_copy(
            src_ref=sq_out.at[pb, d],
            dst_ref=sq_in.at[pb, d],
            send_sem=sq_send.at[d, pb],
            recv_sem=sq_recv.at[d, pb],
            device_id={"ra": of_side(d)[1]},
            device_id_type=MESH,
        )

    def hidden_copy(i):
        return pltpu.make_async_remote_copy(
            src_ref=hidden.at[i],
            dst_ref=hidden.at[i],
            send_sem=hid_send.at[i],
            recv_sem=hid_recv.at[i],
            device_id={"ra": of_side(lax.rem(i, 2))[2]},
            device_id_type=MESH,
        )

    def squares_went(d, pb):
        return (pieces > 1) | (lax.rem(pb, 2) == d)

    def pair_copy(pb):
        return pltpu.make_async_remote_copy(
            src_ref=pair_out.at[pb],
            dst_ref=pair_in.at[pb],
            send_sem=pair_send.at[pb],
            recv_sem=pair_recv.at[pb],
            device_id={"cb": c + 1 - 2 * side},
            device_id_type=MESH,
        )

    def across_copy(pb, k):
        return pltpu.make_async_remote_copy(
            src_ref=shares.at[pb, spot],
            dst_ref=shares.at[pb, spot],
            send_sem=rs_send.at[pb, k - 1],
            recv_sem=rs_recv.at[pb, k - 1],
            device_id={"cb": 2 * lax.rem(spot + k, X) + side},
            device_id_type=MESH,
        )

    def spread_copy(pb):
        return pltpu.make_async_remote_copy(
            src_ref=merged.at[pb, side],
            dst_ref=merged.at[pb, side],
            send_sem=ag_send.at[pb],
            recv_sem=ag_recv.at[pb],
            device_id={"cb": c + 1 - 2 * side},
            device_id_type=MESH,
        )

    def unit_of(i):
        phase = jnp.where(i >= per_phase, 1, 0)
        local = i - phase * per_phase
        return phase, lax.div(local, pieces), lax.rem(local, pieces)

    def grouped(p, size, body):
        left = pieces % size
        if left == 0:
            body(size)
        elif left == pieces:
            body(left)
        else:

            @pl.when(p + size <= pieces)
            def _():
                body(size)

            @pl.when(p + size > pieces)
            def _():
                body(left)

    def project_two(local):
        block = lax.div(local, pieces)
        p = lax.rem(local, pieces)

        def some(size):
            @pl.when(block == 0)
            def _():
                for q in range(size):
                    weight_copy(1, p + q, 0).wait()
                    weight_copy(1, p + q, 1).wait()

            x = normed[block]
            for q in range(size):
                for which in range(2):
                    own[local + q, which] = jnp.dot(
                        x, w_in[1, p + q, which], preferred_element_type=jnp.float32
                    )

        grouped(p, WIDE, some)

    def forward(i, d):
        phase, block, p = unit_of(i)
        place = of_side(d)[0]
        slot = i - phase * per_phase
        pb = phase * blocks + block
        opening = p < 2
        old = i - 2 * BEHIND

        @pl.when((place < R - 1) & (old >= 0))
        def _():
            part_copy(old).wait_send()

        @pl.when(place == 0)
        def _():
            part_out[i] = own[slot].astype(jnp.bfloat16)
            part_copy(i).start()

            @pl.when(opening)
            def _():
                sq_out[pb, d] = sq_own[phase, block]
                square_copy(d, pb).start()

        @pl.when((place > 0) & (place < R - 1))
        def _():
            part_copy(i).wait_recv()
            part_out[i] = (own[slot] + part_in[i].astype(jnp.float32)).astype(jnp.bfloat16)
            part_copy(i).start()

            @pl.when(opening)
            def _():
                square_copy(d, pb).wait_recv()
                sq_out[pb, d] = sq_own[phase, block] + sq_in[pb, d]
                square_copy(d, pb).start()

        @pl.when(place == R - 1)
        def _():
            @pl.when(opening)
            def _():
                square_copy(d, pb).wait_recv()
                mean = (sq_own[phase, block] + sq_in[pb, d])[:1] / model
                line = lax.rsqrt(mean + epsilon)
                column = jnp.sum(jnp.where(diagonal(), line, 0.0), axis=1, keepdims=True)
                scale[d] = jnp.broadcast_to(column, (rows, LANES))

            part_copy(i).wait_recv()
            factor = scale[d][:, :1]
            gate = (own[slot, 0] + part_in[i, 0].astype(jnp.float32)) * factor
            up = (own[slot, 1] + part_in[i, 1].astype(jnp.float32)) * factor
            hidden[i] = (gate / (1.0 + jnp.exp(-gate)) * up).astype(jnp.bfloat16)

    def backward(i, d):
        place = of_side(d)[0]

        @pl.when(place < R - 1)
        def _():
            hidden_copy(i).wait_recv()

        hidden_copy(i).start()

        @pl.when(i >= 2 * BEHIND)
        def _():
            hidden_copy(i - 2 * BEHIND).wait_send()

    steps = -(-pieces // DEEP)

    def down(group):
        pb = lax.div(group, steps)
        phase = jnp.where(pb >= blocks, 1, 0)
        start = lax.rem(group, steps) * DEEP

        def some(size):
            for q in range(size):
                i = pb * pieces + start + q

                @pl.when(of_side(lax.rem(i, 2))[0] == 0)
                def _(i=i):
                    hidden_copy(i).wait_recv()

                @pl.when(pb == 0)
                def _(q=q):
                    weight_copy(0, start + q, 2).wait()
                    weight_copy(1, start + q, 0).start()
                    weight_copy(1, start + q, 1).start()
                    weight_copy(1, start + q, 2).start()

                @pl.when(pb == blocks)
                def _(q=q):
                    weight_copy(1, start + q, 2).wait()

            slot = pb * pieces + start
            product = jnp.dot(
                jnp.concatenate([hidden[slot + q] for q in range(size)], axis=1),
                w_down[phase, pl.ds(start, size)].reshape(size * width, -1),
                preferred_element_type=jnp.float32,
            )

            @pl.when(start == 0)
            def _():
                total[...] = product.reshape(total.shape)

            @pl.when(start > 0)
            def _():
                total[...] += product.reshape(total.shape)

        grouped(start, DEEP, some)

        @pl.when(start + DEEP >= pieces)
        def _():
            pair_own[lax.rem(pb, 2)] = total[side]
            pair_out[pb] = total[1 - side]
            pair_copy(pb).start()
            for d in range(2):

                @pl.when((of_side(d)[0] < R - 1) & squares_went(d, pb))
                def _(d=d):
                    square_copy(d, pb).wait_send()

    def pair(pb):
        pair_copy(pb).wait_recv()
        shares[pb, spot] = (pair_own[lax.rem(pb, 2)] + pair_in[pb]).astype(jnp.bfloat16)
        for k in range(1, X):
            across_copy(pb, k).start()

        @pl.when(pb > 0)
        def _():
            pair_copy(pb - 1).wait_send()

    def across(pb):
        for k in range(1, X):
            across_copy(pb, k).wait_recv()
        branch = shares[pb, 0].astype(jnp.float32)
        for x in range(1, X):
            branch = branch + shares[pb, x].astype(jnp.float32)

        @pl.when(pb < blocks)
        def _():
            values = stream_in[pb, side].astype(jnp.float32)
            merged[pb, side] = (values + 0.5 * branch).astype(jnp.bfloat16)

        @pl.when(pb >= blocks)
        def _():
            values = merged[pb - blocks, side].astype(jnp.float32)
            merged[pb, side] = (values + 0.5 * branch).astype(jnp.bfloat16)

        spread_copy(pb).start()

        @pl.when(pb > 0)
        def _():
            for k in range(1, X):
                across_copy(pb - 1, k).wait_send()
            spread_copy(pb - 1).wait_send()

    def settle(pb):
        spread_copy(pb).wait_recv()

        @pl.when(pb < blocks)
        def _():
            normed[pb], square = scaled(merged[pb].reshape(rows, -1), gain_two)
            keep_square(1, pb, square)

        @pl.when(pb >= blocks)
        def _():
            out[pb - blocks] = merged[pb]

    bodies = (
        lambda n: forward(2 * n, 0),
        lambda n: forward(2 * n + 1, 1),
        lambda n: backward(2 * n, 0),
        lambda n: backward(2 * n + 1, 1),
        down,
        pair,
        across,
        settle,
        project_one,
        project_two,
    )

    def step(at, counts):
        what = table[at]

        def one(kind):
            def run():
                bodies[kind](counts[kind])
                return counts[kind] + 1

            return lax.cond(what == kind, run, lambda: counts[kind])

        after = []
        for kinds in (range(2), range(2, 4), range(4, 6), range(6, len(bodies))):
            after += lax.cond(
                (what >= kinds[0]) & (what <= kinds[-1]),
                lambda: tuple(one(kind) for kind in kinds),
                lambda: tuple(counts[kind] for kind in kinds),
            )
        return tuple(after)

    done = [min(FIRST, pieces) if body is project_one else 0 for body in bodies]
    lax.fori_loop(0, length, step, tuple(jnp.int32(n) for n in done))

    for i in range(max(0, count - 2 * BEHIND), count):
        place = of_side(i % 2)[0]

        @pl.when(place < R - 1)
        def _(i=i):
            part_copy(i).wait_send()

        @pl.when(place > 0)
        def _(i=i):
            hidden_copy(i).wait_send()

    newest = 2 * blocks - 1
    pair_copy(newest).wait_send()
    for k in range(1, X):
        across_copy(newest, k).wait_send()
    spread_copy(newest).wait_send()


def solution(mesh):
    R, C = mesh.shape["ra"], mesh.shape["cb"]

    def per_device(
        residual,
        gain_first,
        gate_first,
        up_first,
        down_first,
        gain_second,
        gate_second,
        up_second,
        down_second,
    ):
        tokens, depth = residual.shape
        units = gate_first.shape[1]
        blocks = max(1, min(4, tokens // (16 * C)))
        width = 2 * LANES if units % (2 * LANES) == 0 else units
        pieces = units // width
        rows = tokens // blocks
        count = 2 * blocks * pieces
        half = rows // 2
        orders = plan(R, blocks, pieces, DEEP, WIDE, UNIT)
        length = max(len(order) for order in orders)
        bf16, f32 = jnp.bfloat16, jnp.float32
        vmem = functools.partial(pl.BlockSpec, memory_space=pltpu.VMEM)
        hbm = functools.partial(pl.BlockSpec, memory_space=pl.ANY)
        pbs = 2 * blocks
        dma = pltpu.SemaphoreType.DMA
        result = pl.pallas_call(
            functools.partial(
                kernel, (R, C, blocks, pieces, width, rows, orders, float(depth * R))
            ),
            out_shape=pltpu.VMEM((blocks, 2, half, depth), bf16),
            in_specs=[hbm()] * 9,
            out_specs=vmem(),
            scratch_shapes=[
                pltpu.VMEM((2, pieces, 2, depth, width), bf16),
                pltpu.VMEM((2, pieces, width, depth), bf16),
                pltpu.VMEM((blocks, 2, half, depth), bf16),
                pltpu.VMEM((depth,), bf16),
                pltpu.VMEM((depth,), bf16),
                pltpu.VMEM((tokens, depth), bf16),
                pltpu.VMEM((blocks, rows, depth), bf16),
                pltpu.VMEM((blocks * pieces, 2, rows, width), f32),
                pltpu.VMEM((count, 2, rows, width), bf16),
                pltpu.VMEM((count, 2, rows, width), bf16),
                pltpu.VMEM((count, rows, width), bf16),
                pltpu.VMEM((2, half, depth), f32),
                pltpu.SMEM((length,), jnp.int32),
                pltpu.VMEM((2, half, depth), f32),
                pltpu.VMEM((pbs, half, depth), f32),
                pltpu.VMEM((pbs, half, depth), f32),
                pltpu.VMEM((pbs, C // 2, half, depth), bf16),
                pltpu.VMEM((pbs, 2, half, depth), bf16),
                pltpu.VMEM((2, blocks, TILE, rows), f32),
                pltpu.VMEM((pbs, 2, TILE, rows), f32),
                pltpu.VMEM((pbs, 2, TILE, rows), f32),
                pltpu.VMEM((2, rows, LANES), f32),
                dma((2, 3, pieces)),
                dma,
                dma((2,)),
                dma((count,)),
                dma((count,)),
                dma((count,)),
                dma((count,)),
                dma((2, pbs)),
                dma((2, pbs)),
                dma((pbs,)),
                dma((pbs,)),
                dma((pbs, max(1, C // 2 - 1))),
                dma((pbs, max(1, C // 2 - 1))),
                dma((pbs,)),
                dma((pbs,)),
            ],
            compiler_params=pltpu.CompilerParams(
                collective_id=0, has_side_effects=True, vmem_limit_bytes=66400000
            ),
        )(
            residual.reshape(blocks, 2, half, depth),
            gain_first,
            gain_second,
            gate_first,
            up_first,
            down_first,
            gate_second,
            up_second,
            down_second,
        )
        return result.reshape(tokens, depth)

    in_specs = (
        P("grp", "ra"),
        P("ra"),
        P("ra", "cb"),
        P("ra", "cb"),
        P("cb", "ra"),
        P("ra"),
        P("ra", "cb"),
        P("ra", "cb"),
        P("cb", "ra"),
    )
    return jax.shard_map(
        per_device, mesh=mesh, in_specs=in_specs, out_specs=P("grp", "ra"), check_vma=False
    )
```

```python
import functools
import heapq

import jax
import jax.numpy as jnp
from jax import lax
from jax.experimental import pallas as pl
from jax.experimental.pallas import tpu as pltpu
from jax.sharding import PartitionSpec as P

MESH = pl.DeviceIdType.MESH
LANES = 128
epsilon = 1e-06

TILE = 8
AHEAD = 3
BEHIND = 4
WIDE = 1
FIRST = 2
DEEP = 4
UNIT = 1.405

FORWARD, BACKWARD, DOWN, PAIR, ACROSS, SETTLE, PROJECT_ONE, PROJECT_TWO, REST = 0, 2, 4, 5, 6, 7, 8, 9, 10
COST = {
    "op": 0.12, "forward": 0.1, "finish": 0.16, "backward": 0.02, "down": 0.16, "project_one": 0.45,
    "project_two": 0.3, "pair": 0.1, "across": 0.1, "settle": 0.2, "hop": 2.2, "near": 1.8, "far": 4.2,
    "queue": 2.0, "bubble": 0.05,
}
RANK = {
    "settle": 0.5, "across": 0.6, "pair": 0.7, "backward0": 2, "forward1": 2.5, "forward0": 3,
    "project_one": 3.6, "down0": 4, "backward1": 4.75, "project_two": 5.2, "down1": 6.4,
}


def plan(R, blocks, pieces, deep, wide, busy, cost=COST, rank=RANK):
    per_phase = blocks * pieces
    count = 2 * per_phase
    heap = []
    ticket = 0
    groups = []
    for pb in range(2 * blocks):
        for start in range(0, pieces, deep):
            groups.append((pb, start, min(deep, pieces - start)))
    wides = []
    for block in range(blocks):
        for start in range(0, pieces, wide):
            wides.append((block, start, min(wide, pieces - start)))
    units = [[i for i in range(count) if i % 2 == d] for d in range(2)]
    nodes = []
    for z in range(R):
        nodes.append(dict(
            time=0.0, own={b * pieces + p for b in range(blocks) for p in range(min(FIRST, pieces))}, forward=[0, 0], backward=[0, 0], down=0, pair=0, across=0, settle=0,
            one=min(FIRST, pieces), two=0, sums=set(), hidden=set(), done=set(), near={}, far={}, back={}, order=[],
        ))
    free = {}
    sent = {}

    def poke(time, z):
        nonlocal ticket
        ticket += 1
        heapq.heappush(heap, (time, ticket, "try", z, None))

    def land(time, z, where, key):
        nonlocal ticket
        ticket += 1
        heapq.heappush(heap, (time, ticket, where, z, key))

    for z in range(R):
        poke(0.0, z)
        for p in range(pieces):
            poke(0.3 * (p + 1), z)
    while heap:
        now, _, event, z, key = heapq.heappop(heap)
        node = nodes[z]
        if event != "try":
            if event in ("sums", "hidden"):
                node[event].add(key)
            else:
                node[event][key] = now
        if node["time"] > now + 1e-9:
            continue
        place = (z, R - 1 - z)
        best = None

        def offer(name, kind, value, duration):
            nonlocal best
            if best is None or rank[name] < best[0]:
                best = (rank[name], kind, value, duration)

        wake = []

        def open_link(way):
            until = free.get((z, way), 0.0) - cost["queue"]
            if until > now + 1e-9:
                wake.append(until)
                return False
            return True

        for d in range(2):
            way = 1 - 2 * d
            at = node["forward"][d]
            if at < len(units[d]):
                i = units[d][at]
                if i in node["own"] and (place[d] == 0 or i in node["sums"]):
                    phase = i // per_phase
                    if place[d] == R - 1:
                        offer("forward%d" % phase, FORWARD, i, cost["finish"])
                    elif open_link(way):
                        offer("forward%d" % phase, FORWARD, i, cost["forward"])
            at = node["backward"][d]
            if place[d] > 0 and at < len(units[d]):
                i = units[d][at]
                if i in (node["done"] if place[d] == R - 1 else node["hidden"]) and open_link(-way):
                    offer("backward%d" % (i // per_phase), BACKWARD, i, cost["backward"])
        if node["down"] < len(groups):
            pb, start, size = groups[node["down"]]
            ready = True
            for i in range(pb * pieces + start, pb * pieces + start + size):
                d = i % 2
                if place[d] == 0:
                    ready &= i in node["hidden"]
                elif place[d] == R - 1:
                    ready &= i in node["done"]
                else:
                    ready &= units[d].index(i) < node["backward"][d]
            if ready:
                offer("down%d" % (pb // blocks), DOWN, node["down"], cost["down"] * size)
        for name, kind, source in (("pair", PAIR, "near"), ("across", ACROSS, "far"), ("settle", SETTLE, "back")):
            if node[source].get(node[name], 1e9) <= now + 1e-9:
                offer(name, kind, node[name], cost[name])
        if node["one"] < pieces and 0.3 * (node["one"] + 1) <= now + 1e-9:
            offer("project_one", PROJECT_ONE, node["one"], cost["project_one"])
        if node["two"] < len(wides):
            block, start, size = wides[node["two"]]
            if node["settle"] > block:
                offer("project_two", PROJECT_TWO, block * pieces + start, cost["project_two"] * size)
        if best is None:
            for until in wake:
                poke(until, z)
            continue
        _, kind, value, duration = best
        node["order"].append(kind + value % 2 if kind in (FORWARD, BACKWARD) else kind)
        end = now + cost["op"] + duration
        node["time"] = end

        def send(way, size, where, i):
            begin = max(end, free.get((z, way), 0.0))
            free[(z, way)] = begin + size + cost["bubble"]
            land(free[(z, way)] + cost["hop"], z + way, where, i)

        if kind in (FORWARD, BACKWARD):
            d = value % 2
            way = 1 - 2 * d
            if kind == FORWARD:
                node["forward"][d] += 1
                if place[d] == R - 1:
                    node["done"].add(value)
                else:
                    send(way, busy, "sums", value)
            else:
                node["backward"][d] += 1
                send(-way, busy / 2, "hidden", value)
        elif kind == DOWN:
            pb, start, size = groups[value]
            node["down"] += 1
            if start + size == pieces:
                land(end + cost["near"], z, "near", pb)
        elif kind == PAIR:
            node["pair"] += 1
            land(end + cost["far"], z, "far", value)
        elif kind == ACROSS:
            node["across"] += 1
            land(end + cost["near"], z, "back", value)
        elif kind == SETTLE:
            node["settle"] += 1
        elif kind == PROJECT_ONE:
            node["one"] += 1
            node["own"].update(block * pieces + value for block in range(blocks))
        else:
            block, start, size = wides[node["two"]]
            node["two"] += 1
            node["own"].update(per_phase + value + q for q in range(size))
        poke(end, z)
    for node in nodes:
        assert node["settle"] == 2 * blocks
    orders = [node["order"] for node in nodes]
    return orders


def kernel(
    cfg,
    residual,
    gain_first,
    gain_second,
    gate_first,
    up_first,
    down_first,
    gate_second,
    up_second,
    down_second,
    out,
    w_in,
    w_down,
    stream_in,
    gain_one,
    gain_two,
    normed_one,
    normed,
    own,
    part_out,
    part_in,
    hidden,
    total,
    table,
    pair_own,
    pair_out,
    pair_in,
    shares,
    merged,
    sq_own,
    sq_out,
    sq_in,
    scale,
    w_sem,
    x_sem,
    gain_sem,
    part_send,
    part_recv,
    hid_send,
    hid_recv,
    sq_send,
    sq_recv,
    pair_send,
    pair_recv,
    rs_send,
    rs_recv,
    ag_send,
    ag_recv,
):
    R, C, blocks, pieces, width, rows, orders, model = cfg
    per_phase = blocks * pieces
    count = 2 * per_phase
    r = lax.axis_index("ra")
    c = lax.axis_index("cb")
    X = C // 2
    side, spot = lax.rem(c, 2), lax.div(c, 2)
    half = rows // 2
    length = max(len(order) for order in orders)

    gates, ups, downs = (gate_first, gate_second), (up_first, up_second), (down_first, down_second)

    def weight_copy(phase, p, which):
        span = pl.ds(p * width if pieces > 1 else 0, width)
        if which == 2:
            return pltpu.make_async_copy(
                downs[phase].at[span, :], w_down.at[phase, p], w_sem.at[phase, 2, p]
            )
        source = (gates, ups)[which][phase]
        return pltpu.make_async_copy(
            source.at[:, span], w_in.at[phase, p, which], w_sem.at[phase, which, p]
        )

    stream_copy = pltpu.make_async_copy(residual, stream_in, x_sem)
    stream_copy.start()
    gain_copies = [
        pltpu.make_async_copy(source, kept, gain_sem.at[at])
        for at, (source, kept) in enumerate(((gain_first, gain_one), (gain_second, gain_two)))
    ]
    gain_copies[0].start()
    gain_copies[1].start()
    for p in range(min(AHEAD, pieces)):
        weight_copy(0, p, 0).start()
        weight_copy(0, p, 1).start()

    for z, order in enumerate(orders):

        @pl.when(r == z)
        def _(order=order):
            for at, kind in enumerate(order):
                table[at] = kind
            for at in range(len(order), length):
                table[at] = REST

    barrier = pltpu.get_barrier_semaphore()

    @pl.when(r > 0)
    def _():
        pl.semaphore_signal(barrier, inc=1, device_id={"ra": r - 1}, device_id_type=MESH)

    @pl.when(r < R - 1)
    def _():
        pl.semaphore_signal(barrier, inc=1, device_id={"ra": r + 1}, device_id_type=MESH)

    for k in range(1, C):
        pl.semaphore_signal(
            barrier, inc=1, device_id={"cb": lax.rem(c + k, C)}, device_id_type=MESH
        )

    def diagonal():
        shape = (rows, rows)
        return lax.broadcasted_iota(jnp.int32, shape, 0) == lax.broadcasted_iota(jnp.int32, shape, 1)

    def scaled(stream, gain_ref):
        values = stream.astype(jnp.float32)
        square = jnp.sum(values * values, axis=1, keepdims=True)
        gain = gain_ref[...].astype(jnp.float32).reshape(1, -1)
        return (values * gain).astype(jnp.bfloat16), square

    def keep_square(phase, block, square):
        line = jnp.sum(jnp.where(diagonal(), square, 0.0), axis=0, keepdims=True)
        sq_own[phase, block] = jnp.broadcast_to(line, (TILE, rows))

    stream_copy.wait()
    gain_copies[0].wait()
    gain_copies[1].wait()
    for block in range(blocks):
        normed_one[pl.ds(block * rows, rows)], square = scaled(
            stream_in[block].reshape(rows, -1), gain_one
        )
        keep_square(0, block, square)

    def project_one(p):
        @pl.when(p + AHEAD < pieces)
        def _():
            weight_copy(0, p + AHEAD, 0).start()
            weight_copy(0, p + AHEAD, 1).start()

        weight_copy(0, p, 2).start()
        for which in range(2):
            weight_copy(0, p, which).wait()
        x = normed_one[...]
        for which in range(2):
            product = jnp.dot(x, w_in[0, p, which], preferred_element_type=jnp.float32)
            for block in range(blocks):
                own[block * pieces + p, which] = product[block * rows : (block + 1) * rows]

    for p in range(min(FIRST, pieces)):
        project_one(p)

    near = jnp.where(r > 0, 1, 0) + jnp.where(r < R - 1, 1, 0)
    pl.semaphore_wait(barrier, C - 1 + near)

    def of_side(d):
        rise = d == 0
        place = jnp.where(rise, r, R - 1 - r)
        return place, jnp.where(rise, r + 1, r - 1), jnp.where(rise, r - 1, r + 1)

    def part_copy(i):
        return pltpu.make_async_remote_copy(
            src_ref=part_out.at[i],
            dst_ref=part_in.at[i],
            send_sem=part_send.at[i],
            recv_sem=part_recv.at[i],
            device_id={"ra": of_side(lax.rem(i, 2))[1]},
            device_id_type=MESH,
        )

    def square_copy(d, pb):
        return pltpu.make_async_remote_copy(
            src_ref=sq_out.at[pb, d],
            dst_ref=sq_in.at[pb, d],
            send_sem=sq_send.at[d, pb],
            recv_sem=sq_recv.at[d, pb],
            device_id={"ra": of_side(d)[1]},
            device_id_type=MESH,
        )

    def hidden_copy(i):
        return pltpu.make_async_remote_copy(
            src_ref=hidden.at[i],
            dst_ref=hidden.at[i],
            send_sem=hid_send.at[i],
            recv_sem=hid_recv.at[i],
            device_id={"ra": of_side(lax.rem(i, 2))[2]},
            device_id_type=MESH,
        )

    def squares_went(d, pb):
        return (pieces > 1) | (lax.rem(pb, 2) == d)

    def pair_copy(pb):
        return pltpu.make_async_remote_copy(
            src_ref=pair_out.at[pb],
            dst_ref=pair_in.at[pb],
            send_sem=pair_send.at[pb],
            recv_sem=pair_recv.at[pb],
            device_id={"cb": c + 1 - 2 * side},
            device_id_type=MESH,
        )

    def across_copy(pb, k):
        return pltpu.make_async_remote_copy(
            src_ref=shares.at[pb, spot],
            dst_ref=shares.at[pb, spot],
            send_sem=rs_send.at[pb, k - 1],
            recv_sem=rs_recv.at[pb, k - 1],
            device_id={"cb": 2 * lax.rem(spot + k, X) + side},
            device_id_type=MESH,
        )

    def spread_copy(pb):
        return pltpu.make_async_remote_copy(
            src_ref=merged.at[pb, side],
            dst_ref=merged.at[pb, side],
            send_sem=ag_send.at[pb],
            recv_sem=ag_recv.at[pb],
            device_id={"cb": c + 1 - 2 * side},
            device_id_type=MESH,
        )

    def unit_of(i):
        phase = jnp.where(i >= per_phase, 1, 0)
        local = i - phase * per_phase
        return phase, lax.div(local, pieces), lax.rem(local, pieces)

    def grouped(p, size, body):
        left = pieces % size
        if left == 0:
            body(size)
        elif left == pieces:
            body(left)
        else:

            @pl.when(p + size <= pieces)
            def _():
                body(size)

            @pl.when(p + size > pieces)
            def _():
                body(left)

    def project_two(local):
        block = lax.div(local, pieces)
        p = lax.rem(local, pieces)

        def some(size):
            @pl.when(block == 0)
            def _():
                for q in range(size):
                    weight_copy(1, p + q, 0).wait()
                    weight_copy(1, p + q, 1).wait()

            x = normed[block]
            for q in range(size):
                for which in range(2):
                    own[local + q, which] = jnp.dot(
                        x, w_in[1, p + q, which], preferred_element_type=jnp.float32
                    )

        grouped(p, WIDE, some)

    def forward(i, d):
        phase, block, p = unit_of(i)
        place = of_side(d)[0]
        slot = i - phase * per_phase
        pb = phase * blocks + block
        opening = p < 2
        old = i - 2 * BEHIND

        @pl.when((place < R - 1) & (old >= 0))
        def _():
            part_copy(old).wait_send()

        @pl.when(place == 0)
        def _():
            part_out[i] = own[slot].astype(jnp.bfloat16)
            part_copy(i).start()

            @pl.when(opening)
            def _():
                sq_out[pb, d] = sq_own[phase, block]
                square_copy(d, pb).start()

        @pl.when((place > 0) & (place < R - 1))
        def _():
            part_copy(i).wait_recv()
            part_out[i] = (own[slot] + part_in[i].astype(jnp.float32)).astype(jnp.bfloat16)
            part_copy(i).start()

            @pl.when(opening)
            def _():
                square_copy(d, pb).wait_recv()
                sq_out[pb, d] = sq_own[phase, block] + sq_in[pb, d]
                square_copy(d, pb).start()

        @pl.when(place == R - 1)
        def _():
            @pl.when(opening)
            def _():
                square_copy(d, pb).wait_recv()
                mean = (sq_own[phase, block] + sq_in[pb, d])[:1] / model
                line = lax.rsqrt(mean + epsilon)
                column = jnp.sum(jnp.where(diagonal(), line, 0.0), axis=1, keepdims=True)
                scale[d] = jnp.broadcast_to(column, (rows, LANES))

            part_copy(i).wait_recv()
            factor = scale[d][:, :1]
            gate = (own[slot, 0] + part_in[i, 0].astype(jnp.float32)) * factor
            up = (own[slot, 1] + part_in[i, 1].astype(jnp.float32)) * factor
            hidden[i] = (gate / (1.0 + jnp.exp(-gate)) * up).astype(jnp.bfloat16)

    def backward(i, d):
        place = of_side(d)[0]

        @pl.when(place < R - 1)
        def _():
            hidden_copy(i).wait_recv()

        hidden_copy(i).start()

        @pl.when(i >= 2 * BEHIND)
        def _():
            hidden_copy(i - 2 * BEHIND).wait_send()

    steps = -(-pieces // DEEP)

    def down(group):
        pb = lax.div(group, steps)
        phase = jnp.where(pb >= blocks, 1, 0)
        start = lax.rem(group, steps) * DEEP

        def some(size):
            for q in range(size):
                i = pb * pieces + start + q

                @pl.when(of_side(lax.rem(i, 2))[0] == 0)
                def _(i=i):
                    hidden_copy(i).wait_recv()

                @pl.when(pb == 0)
                def _(q=q):
                    weight_copy(0, start + q, 2).wait()
                    weight_copy(1, start + q, 0).start()
                    weight_copy(1, start + q, 1).start()
                    weight_copy(1, start + q, 2).start()

                @pl.when(pb == blocks)
                def _(q=q):
                    weight_copy(1, start + q, 2).wait()

            slot = pb * pieces + start
            product = jnp.dot(
                jnp.concatenate([hidden[slot + q] for q in range(size)], axis=1),
                w_down[phase, pl.ds(start, size)].reshape(size * width, -1),
                preferred_element_type=jnp.float32,
            )

            @pl.when(start == 0)
            def _():
                total[...] = product.reshape(total.shape)

            @pl.when(start > 0)
            def _():
                total[...] += product.reshape(total.shape)

        grouped(start, DEEP, some)

        @pl.when(start + DEEP >= pieces)
        def _():
            pair_own[lax.rem(pb, 2)] = total[side]
            pair_out[pb] = total[1 - side]
            pair_copy(pb).start()
            for d in range(2):

                @pl.when((of_side(d)[0] < R - 1) & squares_went(d, pb))
                def _(d=d):
                    square_copy(d, pb).wait_send()

    def pair(pb):
        pair_copy(pb).wait_recv()
        shares[pb, spot] = (pair_own[lax.rem(pb, 2)] + pair_in[pb]).astype(jnp.bfloat16)
        for k in range(1, X):
            across_copy(pb, k).start()

        @pl.when(pb > 0)
        def _():
            pair_copy(pb - 1).wait_send()

    def across(pb):
        for k in range(1, X):
            across_copy(pb, k).wait_recv()
        branch = shares[pb, 0].astype(jnp.float32)
        for x in range(1, X):
            branch = branch + shares[pb, x].astype(jnp.float32)

        @pl.when(pb < blocks)
        def _():
            values = stream_in[pb, side].astype(jnp.float32)
            merged[pb, side] = (values + 0.5 * branch).astype(jnp.bfloat16)

        @pl.when(pb >= blocks)
        def _():
            values = merged[pb - blocks, side].astype(jnp.float32)
            merged[pb, side] = (values + 0.5 * branch).astype(jnp.bfloat16)

        spread_copy(pb).start()

        @pl.when(pb > 0)
        def _():
            for k in range(1, X):
                across_copy(pb - 1, k).wait_send()
            spread_copy(pb - 1).wait_send()

    def settle(pb):
        spread_copy(pb).wait_recv()

        @pl.when(pb < blocks)
        def _():
            normed[pb], square = scaled(merged[pb].reshape(rows, -1), gain_two)
            keep_square(1, pb, square)

        @pl.when(pb >= blocks)
        def _():
            out[pb - blocks] = merged[pb]

    bodies = (
        lambda n: forward(2 * n, 0),
        lambda n: forward(2 * n + 1, 1),
        lambda n: backward(2 * n, 0),
        lambda n: backward(2 * n + 1, 1),
        down,
        pair,
        across,
        settle,
        project_one,
        project_two,
    )

    def step(at, counts):
        what = table[at]

        def one(kind):
            def run():
                bodies[kind](counts[kind])
                return counts[kind] + 1

            return lax.cond(what == kind, run, lambda: counts[kind])

        def some(*parts):
            kinds = [kind for part in parts for kind in part]

            def run():
                if len(parts) == 1:
                    return tuple(one(kind) for kind in kinds)
                return sum((some(part) for part in parts), ())

            return tuple(
                lax.cond(
                    (what >= kinds[0]) & (what <= kinds[-1]),
                    run,
                    lambda: tuple(counts[kind] for kind in kinds),
                )
            )

        return some(range(2), range(2, 4)) + some(range(4, 6), range(6, 8), range(8, len(bodies)))

    done = [min(FIRST, pieces) if body is project_one else 0 for body in bodies]
    lax.fori_loop(0, length, step, tuple(jnp.int32(n) for n in done))

    for i in range(max(0, count - 2 * BEHIND), count):
        place = of_side(i % 2)[0]

        @pl.when(place < R - 1)
        def _(i=i):
            part_copy(i).wait_send()

        @pl.when(place > 0)
        def _(i=i):
            hidden_copy(i).wait_send()

    newest = 2 * blocks - 1
    pair_copy(newest).wait_send()
    for k in range(1, X):
        across_copy(newest, k).wait_send()
    spread_copy(newest).wait_send()


def solution(mesh):
    R, C = mesh.shape["ra"], mesh.shape["cb"]

    def per_device(
        residual,
        gain_first,
        gate_first,
        up_first,
        down_first,
        gain_second,
        gate_second,
        up_second,
        down_second,
    ):
        tokens, depth = residual.shape
        units = gate_first.shape[1]
        blocks = max(1, min(4, tokens // (16 * C)))
        width = 2 * LANES if units % (2 * LANES) == 0 else units
        pieces = units // width
        rows = tokens // blocks
        count = 2 * blocks * pieces
        half = rows // 2
        orders = plan(R, blocks, pieces, DEEP, WIDE, UNIT)
        length = max(len(order) for order in orders)
        bf16, f32 = jnp.bfloat16, jnp.float32
        vmem = functools.partial(pl.BlockSpec, memory_space=pltpu.VMEM)
        hbm = functools.partial(pl.BlockSpec, memory_space=pl.ANY)
        pbs = 2 * blocks
        dma = pltpu.SemaphoreType.DMA
        result = pl.pallas_call(
            functools.partial(
                kernel, (R, C, blocks, pieces, width, rows, orders, float(depth * R))
            ),
            out_shape=pltpu.VMEM((blocks, 2, half, depth), bf16),
            in_specs=[hbm()] * 9,
            out_specs=vmem(),
            scratch_shapes=[
                pltpu.VMEM((2, pieces, 2, depth, width), bf16),
                pltpu.VMEM((2, pieces, width, depth), bf16),
                pltpu.VMEM((blocks, 2, half, depth), bf16),
                pltpu.VMEM((depth,), bf16),
                pltpu.VMEM((depth,), bf16),
                pltpu.VMEM((tokens, depth), bf16),
                pltpu.VMEM((blocks, rows, depth), bf16),
                pltpu.VMEM((blocks * pieces, 2, rows, width), f32),
                pltpu.VMEM((count, 2, rows, width), bf16),
                pltpu.VMEM((count, 2, rows, width), bf16),
                pltpu.VMEM((count, rows, width), bf16),
                pltpu.VMEM((2, half, depth), f32),
                pltpu.SMEM((length,), jnp.int32),
                pltpu.VMEM((2, half, depth), f32),
                pltpu.VMEM((pbs, half, depth), f32),
                pltpu.VMEM((pbs, half, depth), f32),
                pltpu.VMEM((pbs, C // 2, half, depth), bf16),
                pltpu.VMEM((pbs, 2, half, depth), bf16),
                pltpu.VMEM((2, blocks, TILE, rows), f32),
                pltpu.VMEM((pbs, 2, TILE, rows), f32),
                pltpu.VMEM((pbs, 2, TILE, rows), f32),
                pltpu.VMEM((2, rows, LANES), f32),
                dma((2, 3, pieces)),
                dma,
                dma((2,)),
                dma((count,)),
                dma((count,)),
                dma((count,)),
                dma((count,)),
                dma((2, pbs)),
                dma((2, pbs)),
                dma((pbs,)),
                dma((pbs,)),
                dma((pbs, max(1, C // 2 - 1))),
                dma((pbs, max(1, C // 2 - 1))),
                dma((pbs,)),
                dma((pbs,)),
            ],
            compiler_params=pltpu.CompilerParams(
                collective_id=0, has_side_effects=True, vmem_limit_bytes=66400000
            ),
        )(
            residual.reshape(blocks, 2, half, depth),
            gain_first,
            gain_second,
            gate_first,
            up_first,
            down_first,
            gate_second,
            up_second,
            down_second,
        )
        return result.reshape(tokens, depth)

    in_specs = (
        P("grp", "ra"),
        P("ra"),
        P("ra", "cb"),
        P("ra", "cb"),
        P("cb", "ra"),
        P("ra"),
        P("ra", "cb"),
        P("ra", "cb"),
        P("cb", "ra"),
    )
    return jax.shard_map(
        per_device, mesh=mesh, in_specs=in_specs, out_specs=P("grp", "ra"), check_vma=False
    )
```
